32 devices in a mesh: ep: 8 (over z, x), tp: 4 (over y, core).
Axes of the slice: x: 2, y: 2, z: 4, core: 2. Of those that a mesh axis runs over, the one named last changes fastest.
Arguments:
- tokens_first: bfloat16 [4096, 2048], P('ep'), may hold values from -6 to 6
- attn_gain: float32 [2048], replicated, may hold values from 0.1 to 1.9
- w_query: bfloat16 [2048, 1024], P(None, 'tp'), may hold values from -6 to 6
- key_matrix: bfloat16 [2048, 512], P(None, 'tp'), may hold values from -6 to 6
- value_matrix: bfloat16 [2048, 512], P(None, 'tp'), may hold values from -0.125 to 0.125
- head_sink_logit: float32 [16], P('tp'), may hold values from 1 to 5
- w_output: bfloat16 [1024, 2048], P('tp'), may hold values from -0.75 to 0.75
- tokens_second: bfloat16 [1024, 2048], P('ep'), may hold values from -6 to 6
- ffn_gain: float32 [2048], replicated, may hold values from 0.1 to 1.9
- routes: int32 [1024, 4], P('ep'), may hold values from 0 to 15, all different within a row; in each aligned block of 128 rows (0 to 127, 128 to 255, ...) at most 64 rows name the same one
- route_weight: float32 [1024, 4], P('ep'), may hold values from 0.2 to 1.5
- w_gate_exp: bfloat16 [16, 2048, 2048], P('ep', None, 'tp'), may hold values from -0.125 to 0.125
- w_up_exp: bfloat16 [16, 2048, 2048], P('ep', None, 'tp'), may hold values from -0.125 to 0.125
- w_down_exp: bfloat16 [16, 2048, 2048], P('ep', 'tp'), may hold values from -0.125 to 0.125
- w_gate_shared: bfloat16 [2048, 1024], P(None, 'tp'), may hold values from -0.125 to 0.125
- w_up_shared: bfloat16 [2048, 1024], P(None, 'tp'), may hold values from -0.125 to 0.125
- w_down_shared: bfloat16 [1024, 2048], P('tp'), may hold values from -0.1875 to 0.1875
Outputs:
- mixer_out: bfloat16 [4096, 2048], P(('ep', 'tp'))
- moe_out: bfloat16 [1024, 2048], P('ep', 'tp')
The draws below stay inside these ranges and needn't reach their ends.
Inputs may be any that keep to these rules, and one draw needn't show every extreme that they name: `routes`: each row names 4 different experts; among the rows of one index of ep no expert is named more than 64 times, a bound that some block reaches.
All inputs are finite; a program needn't handle non-finite values.
Results may differ from the reference program's by a relative error of at most 0.017.
Values may be sent and summed in bfloat16 or wider, within the bound.
No kernel may reach another device: no remote copies, remote signals or barrier semaphores. Data moves between devices by JAX's collectives and lax.ppermute only.
A program may use at most 64 MiB of HBM per device.

```python
import math
import jax
import jax.numpy as jnp
import numpy as np
from jax import lax

MODEL_WIDTH = 2048
HEAD_SIZE = 64
QUERY_HEADS = 16
KEY_VALUE_HEADS = 8
BAND_LENGTH = 128
EFF = 2048
SFF = 1024
TOPK = 4
TOK1_DEV = 512
TOK2_DEV = 128
EXPERTS = 16
CAP = 64
TOKENS1 = 4096
TOKENS2 = 1024
N_EP = 8
N_TP = 4


def key_lookup(key):
    rotary_base = jax.random.normal(jax.random.fold_in(key, 7), (MODEL_WIDTH, KEY_VALUE_HEADS * HEAD_SIZE), jnp.float32)
    return jnp.clip(rotary_base, -6.0, 6.0) / math.sqrt(MODEL_WIDTH)


def draw_key_matrix(key, part):
    return key_lookup(key).astype(jnp.bfloat16)


def draw_w_query(key, part):
    rotary_base = jnp.clip(jax.random.normal(jax.random.fold_in(key, 11), (MODEL_WIDTH, QUERY_HEADS * HEAD_SIZE), jnp.float32), -6.0, 6.0) / math.sqrt(MODEL_WIDTH)
    return jnp.clip(rotary_base, -6.0, 6.0).astype(jnp.bfloat16)


def shard_levels(stream_key, dims, pieces, smallest, high):
    loudness = 1.0
    for position, shards_of in pieces:
        heights = jax.random.uniform(jax.random.fold_in(jax.random.fold_in(stream_key, 6), position), (shards_of,), jnp.float32, smallest / len(pieces), high / len(pieces))
        loudness = loudness * jnp.repeat(jnp.exp(heights), dims[position] // shards_of).reshape((-1,) + (1,) * (len(dims) - 1 - position))
    return loudness


def assign_block(key, own, number, rows, number_of, top, most, lean):
    ranking = jax.random.permutation(key, number_of)
    crowded, ordinary = portions_of(number_of, rows * top, most, lean, True), portions_of(number_of, rows * top, most, lean, False)
    places = jnp.arange(number_of)

    def named(tallies, offset_by):
        used = int((tallies > 0).sum())
        fixed = max(1, used // 4)
        shifted = fixed + (places - fixed + offset_by * (used - fixed)) % max(1, number_of - fixed)
        return jnp.zeros((number_of,), jnp.int32).at[ranking[jnp.where(places < fixed, places, shifted)]].set(jnp.asarray(tallies, jnp.int32))

    tallies = jnp.where(number % 4 == 0, named(crowded, number // 4), named(ordinary, number - number // 4 - 1))
    mixed = jax.random.permutation(jax.random.fold_in(own, 3), number_of)
    source_of, receiver = mixed[0:number_of // 2 * 2:2], mixed[1:number_of // 2 * 2:2]
    margin = jnp.minimum(tallies[source_of] - 1, most - tallies[receiver]) // 2
    margin = jnp.where((source_of == ranking[0]) | (receiver == ranking[0]) | (tallies[receiver] == 0), 0, jnp.maximum(margin, 0))
    shifted = jax.random.randint(jax.random.fold_in(own, 4), (number_of // 2,), 0, 1 << 20) % (margin + 1)
    tallies = tallies.at[source_of].add(-shifted).at[receiver].add(shifted)
    labels = jnp.searchsorted(jnp.cumsum(tallies), jnp.arange(rows * top), side="right").astype(jnp.int32)
    listing = labels.reshape(top, rows).T
    listing = listing[jax.random.permutation(jax.random.fold_in(own, 1), rows)]
    offset_by = jax.random.randint(jax.random.fold_in(own, 2), (rows, 1), 0, top)
    return jnp.take_along_axis(listing, (jnp.arange(top)[None, :] + offset_by) % top, axis=1)


def portions_of(number_of, total, bound, lean, full):
    portions = [(1 << 20) // math.isqrt(rank ** lean) + 1 for rank in range(1, number_of + 1)]
    largest = bound if full else min(bound, max(-(-total // number_of), total * portions[0] // sum(portions)))
    least = 1 if total - largest >= number_of - 1 else 0
    given, surplus = [largest] + [least] * (number_of - 1), total - largest - least * (number_of - 1)
    while surplus > 0:
        free = [i for i in range(1, number_of) if given[i] < largest] or [i for i in range(1, number_of) if given[i] < bound]
        mass, left = sum([portions[i] for i in free]), surplus
        for i in free:
            extra = min(bound - given[i], max(1, left * portions[i] // mass), surplus)
            given[i] = given[i] + extra
            surplus = surplus - extra
    return np.array(given)


def scatter_about(key, extent, spread, bound, pieces=(), kind=jnp.bfloat16):
    level = shard_levels(key, extent, pieces, -0.22, 0.18) if pieces else 1.0
    values = jax.random.normal(key, extent, jnp.float32) * spread * level
    return jnp.minimum(jnp.maximum(values, -bound), bound).astype(kind)


def setup_inputs(seed: int = 0) -> dict:
    arg_keys = jax.random.split(jax.random.key(seed), 18)
    tokens_first = scatter_about(arg_keys[0], (TOKENS1, MODEL_WIDTH), 1.0, 6.0, ((0, 8),))
    attn_gain = jnp.clip(1.0 + 0.18 * jax.random.normal(arg_keys[1], (MODEL_WIDTH,), jnp.float32), 0.1, 1.9)
    w_query = draw_w_query(jax.random.fold_in(arg_keys[17], 71), 0)
    key_matrix = draw_key_matrix(jax.random.fold_in(arg_keys[17], 71), 0)
    value_matrix = scatter_about(arg_keys[4], (MODEL_WIDTH, KEY_VALUE_HEADS * HEAD_SIZE), MODEL_WIDTH ** -0.5, 0.125, ((1, 4),))
    head_sink_logit = jnp.clip(1.0 + 4.0 * jax.random.uniform(arg_keys[5], (QUERY_HEADS,), jnp.float32) ** shard_levels(arg_keys[5], (QUERY_HEADS,), ((0, 4),), -0.2, 0.2), 1.0, 5.0)
    w_output = scatter_about(arg_keys[6], (QUERY_HEADS * HEAD_SIZE, MODEL_WIDTH), (QUERY_HEADS * HEAD_SIZE // 16) ** -0.5, 0.75, ((0, 4),))
    tokens_second = scatter_about(arg_keys[7], (TOKENS2, MODEL_WIDTH), 1.0, 6.0, ((0, 8),))
    ffn_gain = jnp.clip(1.0 + 0.18 * jax.random.normal(arg_keys[8], (MODEL_WIDTH,), jnp.float32), 0.1, 1.9)
    routes_keys = jax.random.split(jax.random.fold_in(arg_keys[9], 1), TOKENS2 // TOK2_DEV)
    routes_turns = jax.random.permutation(jax.random.fold_in(arg_keys[9], 3), TOKENS2 // TOK2_DEV)
    routes = jax.vmap(lambda own, number: assign_block(jax.random.fold_in(arg_keys[9], 2), own, number, TOK2_DEV, EXPERTS, TOPK, CAP, 2))(routes_keys, routes_turns).reshape((TOKENS2, TOPK))
    route_weight = jnp.clip(0.2 + 1.3 * jax.random.uniform(arg_keys[10], (TOKENS2, TOPK), jnp.float32) ** shard_levels(arg_keys[10], (TOKENS2, TOPK), ((0, 8),), -0.2, 0.2), 0.2, 1.5)
    w_gate_exp = scatter_about(arg_keys[11], (EXPERTS, MODEL_WIDTH, EFF), MODEL_WIDTH ** -0.5, 0.125, ((0, 8), (2, 4)))
    w_up_exp = scatter_about(arg_keys[12], (EXPERTS, MODEL_WIDTH, EFF), MODEL_WIDTH ** -0.5, 0.125, ((0, 8), (2, 4)))
    w_down_exp = scatter_about(arg_keys[13], (EXPERTS, EFF, MODEL_WIDTH), EFF ** -0.5, 0.125, ((0, 8), (1, 4)))
    w_gate_shared = scatter_about(arg_keys[14], (MODEL_WIDTH, SFF), MODEL_WIDTH ** -0.5, 0.125, ((1, 4),))
    w_up_shared = scatter_about(arg_keys[15], (MODEL_WIDTH, SFF), MODEL_WIDTH ** -0.5, 0.125, ((1, 4),))
    w_down_shared = scatter_about(arg_keys[16], (SFF, MODEL_WIDTH), SFF ** -0.5, 0.1875, ((0, 4),))
    return dict(tokens_first=tokens_first, attn_gain=attn_gain, w_query=w_query, key_matrix=key_matrix, value_matrix=value_matrix, head_sink_logit=head_sink_logit, w_output=w_output, tokens_second=tokens_second, ffn_gain=ffn_gain, routes=routes, route_weight=route_weight, w_gate_exp=w_gate_exp, w_up_exp=w_up_exp, w_down_exp=w_down_exp, w_gate_shared=w_gate_shared, w_up_shared=w_up_shared, w_down_shared=w_down_shared)


rope_base = 10000.0
norm_eps = 1e-06

def rms_scale(inputs, gain):
    wide = inputs.astype(jnp.float32)
    scaled = wide * lax.rsqrt(lax.optimization_barrier(jnp.mean(wide * wide, axis=-1, keepdims=True)) + norm_eps)
    return (scaled * gain).astype(jnp.bfloat16)

def apply_rotary(heads, token_positions):
    freqs = rope_base ** (-jnp.arange(0, HEAD_SIZE, 2, dtype=jnp.float32) / HEAD_SIZE)
    angles = token_positions[:, None] * freqs[None, :]
    cosine = jnp.cos(angles)[:, None, :]
    sine = jnp.sin(angles)[:, None, :]
    first_half, second_half = jnp.split(heads, 2, axis=-1)
    return jnp.concatenate([first_half * cosine - second_half * sine, second_half * cosine + first_half * sine], axis=-1)

def group_sum(rows, weights, groups):
    width = rows.shape[1] // groups
    parts = jnp.einsum('rtc,tcd->trd', rows.reshape(rows.shape[0], groups, width).astype(jnp.float32), weights.reshape(groups, width, weights.shape[1]).astype(jnp.float32))
    return lax.optimization_barrier(jnp.sum(parts.astype(jnp.bfloat16).astype(jnp.float32), axis=0))

def reference(tokens_first, attn_gain, w_query, key_matrix, value_matrix, head_sink_logit, w_output, tokens_second, ffn_gain, routes, route_weight, w_gate_exp, w_up_exp, w_down_exp, w_gate_shared, w_up_shared, w_down_shared):
    first_count = tokens_first.shape[0]
    norm_input = rms_scale(tokens_first, attn_gain)
    token_positions = jnp.arange(first_count, dtype=jnp.int32).astype(jnp.float32)
    query_rows = apply_rotary(jnp.dot(norm_input, w_query, preferred_element_type=jnp.float32).reshape(first_count, QUERY_HEADS, HEAD_SIZE), token_positions).astype(jnp.bfloat16)
    key_rows = apply_rotary(jnp.dot(norm_input, key_matrix, preferred_element_type=jnp.float32).reshape(first_count, KEY_VALUE_HEADS, HEAD_SIZE), token_positions).astype(jnp.bfloat16)
    value_rows = jnp.dot(norm_input, value_matrix, preferred_element_type=jnp.float32).astype(jnp.bfloat16).reshape(first_count, KEY_VALUE_HEADS, HEAD_SIZE)
    pad_rows = jnp.zeros((BAND_LENGTH, KEY_VALUE_HEADS, HEAD_SIZE), jnp.bfloat16)
    keys_padded = jnp.concatenate([pad_rows, key_rows], axis=0)
    values_padded = jnp.concatenate([pad_rows, value_rows], axis=0)
    layer_block = min(512, TOK1_DEV)
    head_group = QUERY_HEADS // KEY_VALUE_HEADS
    sink_scores = head_sink_logit.astype(jnp.float32).reshape(KEY_VALUE_HEADS, head_group)[:, :, None, None]

    def attend(index):
        leading_row = index * layer_block
        block_queries = lax.dynamic_slice_in_dim(query_rows, leading_row, layer_block, 0).reshape(layer_block, KEY_VALUE_HEADS, head_group, HEAD_SIZE).astype(jnp.float32)
        key_block = lax.dynamic_slice_in_dim(keys_padded, leading_row, layer_block + BAND_LENGTH, 0).astype(jnp.float32)
        value_block = lax.dynamic_slice_in_dim(values_padded, leading_row, layer_block + BAND_LENGTH, 0).astype(jnp.float32)
        scores = jnp.einsum('qhgd,khd->hgqk', block_queries, key_block) * HEAD_SIZE ** (-0.5)
        query_pos = leading_row + jnp.arange(layer_block, dtype=jnp.int32)
        key_pos = leading_row - BAND_LENGTH + jnp.arange(layer_block + BAND_LENGTH, dtype=jnp.int32)
        offsets = query_pos[:, None] - key_pos[None, :]
        visible = (offsets >= 0) & (offsets < BAND_LENGTH) & (key_pos[None, :] >= 0)
        scores = jnp.where(visible[None, None], scores, -jnp.inf)
        peak = jnp.maximum(lax.optimization_barrier(jnp.max(scores, axis=-1, keepdims=True)), sink_scores)
        expo = jnp.exp(scores - peak)
        total = lax.optimization_barrier(jnp.sum(expo, axis=-1, keepdims=True)) + jnp.exp(sink_scores - peak)
        weights = (expo / total).astype(jnp.bfloat16)
        mixed = jnp.einsum('hgqk,khd->qhgd', weights.astype(jnp.float32), value_block)
        return mixed.astype(jnp.bfloat16).reshape(layer_block, QUERY_HEADS * HEAD_SIZE)
    attended = lax.map(attend, jnp.arange(first_count // layer_block, dtype=jnp.int32)).reshape(first_count, QUERY_HEADS * HEAD_SIZE)

    def project(rows):
        return group_sum(rows, w_output, N_TP).astype(jnp.bfloat16)
    mixer_out = lax.map(project, attended.reshape(N_EP, TOK1_DEV, QUERY_HEADS * HEAD_SIZE)).reshape(first_count, MODEL_WIDTH)
    count_second = tokens_second.shape[0]
    normed_second = rms_scale(tokens_second, ffn_gain)
    flat = routes.reshape(N_EP, TOK2_DEV * TOPK)
    onehot = (flat[:, :, None] == jnp.arange(EXPERTS, dtype=jnp.int32)[None, None, :]).astype(jnp.int32)
    ranks = lax.optimization_barrier(jnp.sum((jnp.cumsum(onehot, axis=1) - onehot) * onehot, axis=-1))
    sources = jnp.arange(N_EP, dtype=jnp.int32)[:, None]
    slots = (flat * (N_EP * CAP) + sources * CAP + ranks).reshape(count_second * TOPK).astype(jnp.int32)
    row_ids = jnp.repeat(jnp.arange(count_second, dtype=jnp.int32), TOPK)
    buffer = jnp.zeros((EXPERTS * N_EP * CAP, MODEL_WIDTH), jnp.bfloat16).at[slots].set(normed_second[row_ids])

    def expert(operands):
        rows, gate_w, up_w, down_w = operands
        gate_pre = jnp.dot(rows, gate_w, preferred_element_type=jnp.float32)
        up_pre = jnp.dot(rows, up_w, preferred_element_type=jnp.float32)
        hidden = (jax.nn.silu(gate_pre) * up_pre).astype(jnp.bfloat16)
        return group_sum(hidden, down_w, N_TP).astype(jnp.bfloat16)
    results = lax.map(expert, (buffer.reshape(EXPERTS, N_EP * CAP, MODEL_WIDTH), w_gate_exp, w_up_exp, w_down_exp)).reshape(-1, MODEL_WIDTH)
    chosen = results[slots].reshape(count_second, TOPK, MODEL_WIDTH).astype(jnp.float32)
    routed = lax.optimization_barrier(jnp.sum(chosen * route_weight.astype(jnp.float32)[:, :, None], axis=1))
    shared_hidden = (jax.nn.silu(jnp.dot(normed_second, w_gate_shared, preferred_element_type=jnp.float32)) * jnp.dot(normed_second, w_up_shared, preferred_element_type=jnp.float32)).astype(jnp.bfloat16)
    shared_sum = group_sum(shared_hidden, w_down_shared, N_TP)
    moe_out = (routed + shared_sum).astype(jnp.bfloat16)
    return (mixer_out, moe_out)
```

```python
import functools

import jax
import jax.numpy as jnp
from jax import lax
from jax.experimental import pallas as pl
from jax.experimental.pallas import tpu as pltpu
from jax.sharding import PartitionSpec as P

MODEL_WIDTH = 2048
HEAD_SIZE = 64
BAND_LENGTH = 128


rope_base = 10000.0
norm_eps = 1e-06


def from_behind(value, axis, by):
    devices = lax.axis_size(axis)
    pairs = [(i, i + by) for i in range(devices) if 0 <= i + by < devices]
    return lax.ppermute(value, axis, pairs)


def rms_scale(inputs, gain):
    wide = inputs.astype(jnp.float32)
    scaled = wide * lax.rsqrt(jnp.mean(wide * wide, axis=-1, keepdims=True) + norm_eps)
    return (scaled * gain).astype(jnp.bfloat16)


def apply_rotary(heads, token_positions):
    freqs = rope_base ** (-jnp.arange(0, HEAD_SIZE, 2, dtype=jnp.float32) / HEAD_SIZE)
    angles = token_positions[:, None] * freqs[None, :]
    cosine = jnp.cos(angles)[:, None, :]
    sine = jnp.sin(angles)[:, None, :]
    first_half, second_half = jnp.split(heads, 2, axis=-1)
    return jnp.concatenate(
        [first_half * cosine - second_half * sine, second_half * cosine + first_half * sine],
        axis=-1,
    )


LANES = 128


def swap(value, ep_bits, tp_bits):
    ep, tp = lax.axis_size("ep"), lax.axis_size("tp")
    pairs = [
        (e * tp + t, (e ^ ep_bits) * tp + (t ^ tp_bits)) for e in range(ep) for t in range(tp)
    ]
    return lax.ppermute(value, ("ep", "tp"), pairs)


def pack_kernel(experts, tp, meta, tokens, gain, routes, weight, whole, half, quarter):
    rows, width = tokens.shape
    wide = tokens[...].astype(jnp.float32)
    scaled = wide * lax.rsqrt(jnp.mean(wide * wide, axis=-1, keepdims=True) + norm_eps)
    whole[:, :width] = (scaled * gain[...]).astype(jnp.bfloat16)
    pad = whole.shape[1] - width
    lane = lax.broadcasted_iota(jnp.int32, (rows, pad), 1)
    named = jnp.where(lane < experts, lane, lane - experts)
    dense = jnp.zeros((rows, pad), jnp.float32)
    for k in range(routes.shape[1]):
        dense = dense + jnp.where(named == routes[:, k : k + 1], weight[:, k : k + 1], 0.0)
    high = dense.astype(jnp.bfloat16).astype(jnp.float32)
    cols = jnp.where(lane < experts, high, jnp.where(lane < 2 * experts, dense - high, 0.0))
    whole[:, width:] = cols.astype(jnp.bfloat16)
    part = rows // 2
    half[...] = whole[pl.ds(pl.multiple_of((meta[0] % 2) * part, part), part), :]
    part = rows // tp
    quarter[...] = whole[pl.ds(pl.multiple_of(meta[0] * part, part), part), :]


def pack(meta, tokens, gain, routes, weight, experts):
    rows, width = tokens.shape
    tp = lax.axis_size("tp")
    total = width + -(-2 * experts // LANES) * LANES
    vmem = pl.BlockSpec(memory_space=pltpu.VMEM)
    return pl.pallas_call(
        functools.partial(pack_kernel, experts, tp),
        out_shape=tuple(
            jax.ShapeDtypeStruct((n, total), jnp.bfloat16) for n in (rows, rows // 2, rows // tp)
        ),
        in_specs=[pl.BlockSpec(memory_space=pltpu.SMEM)] + [vmem] * 4,
        out_specs=(vmem,) * 3,
        cost_estimate=pl.CostEstimate(flops=1 << 26, bytes_accessed=1 << 20, transcendentals=0),
        name="pack",
    )(meta, tokens, gain.reshape(1, -1), routes, weight)


def silu(v):
    return v / (1.0 + jnp.exp(-v))


def expert_kernel(places, steps, exp_dev, experts, shared, half, meta, *refs):
    pieces, refs = refs[: len(places)], refs[len(places) :]
    gate, up, down, refs = refs[0], refs[1], refs[2], refs[3:]
    if shared:
        gate_sh, up_sh, down_sh, refs = refs[0], refs[1], refs[2], refs[3:]
    send, keep, held, hidden, scale, sems = refs[:6]
    step = pl.program_id(0)
    blocks, parts, part, total = held.shape
    rows = blocks * parts * part
    width = gate.shape[1]

    @pl.when(step == 0)
    def _():
        copies = []
        for number, (piece, (xor, columns)) in enumerate(zip(pieces, places)):
            where = meta[0] % parts
            if xor is None:
                target = held.at[0]
            elif blocks == 2 and parts == 2:
                target = held.at[1, where ^ xor]
            else:
                target = held.at[:, where ^ xor, :, columns[0] : columns[1]]
            copies.append(pltpu.make_async_copy(piece, target, sems.at[number]))
        for copy in copies:
            copy.start()
        for copy in copies:
            copy.wait()
        cols = held[:, :, :, width:].reshape(rows, total - width).astype(jnp.float32)
        lane = lax.broadcasted_iota(jnp.int32, cols.shape, 1)
        for j in range(exp_dev):
            mine = meta[1] + j
            chosen = (lane == mine) | (lane == mine + experts)
            scale[j] = jnp.sum(jnp.where(chosen, cols, 0.0), axis=1, keepdims=True) * jnp.ones(
                (1, LANES), jnp.float32
            )
        if shared:
            own = held[0].reshape(parts * part, total)[:, :width]
            hidden_sh = refs[6]
            hidden_sh[...] = (
                silu(jnp.dot(own, gate_sh[...], preferred_element_type=jnp.float32))
                * jnp.dot(own, up_sh[...], preferred_element_type=jnp.float32)
            ).astype(jnp.bfloat16)

    @pl.when(step < steps)
    def _():
        tokens = held[:, :, :, :width].reshape(rows, width)
        opened = jnp.dot(tokens, gate[0], preferred_element_type=jnp.float32)
        lifted = jnp.dot(tokens, up[0], preferred_element_type=jnp.float32)
        weight = scale[step // (steps // exp_dev)][:, :1]
        hidden[step] = (silu(opened) * lifted * weight).astype(jnp.bfloat16)

    @pl.when(step >= steps)
    def _():
        joined = jnp.concatenate([hidden[i] for i in range(steps)], axis=1)
        result = jnp.dot(joined, down[...], preferred_element_type=jnp.float32)
        if shared:
            own = parts * part
            extra = jnp.dot(refs[6][...], down_sh[...], preferred_element_type=jnp.float32)
            result = jnp.concatenate([result[:own] + extra, result[own:]], axis=0)
        result = result.astype(jnp.bfloat16)

        @pl.when(step < steps + half)
        def _():
            send[0] = result

        @pl.when(step >= steps + half)
        def _():
            keep[0] = result


def experts_call(meta, pieces, places, shape, gate, up, down, shared, experts, name):
    exp_dev, width, units = gate.shape
    tp = lax.axis_size("tp")
    chunk = min(256, units)
    per = units // chunk
    steps = exp_dev * per
    blocks, parts, part, total = shape
    rows = blocks * parts * part
    slim = width // tp

    def opening(i, meta):
        i = jnp.minimum(i, steps - 1)
        return (i // per, 0, i % per)

    def closing(i, meta):
        k = jnp.maximum(i - steps, 0)
        g = jnp.where(k < tp // 2, 2 * k + 1, 2 * k - tp)
        return (0, jnp.bitwise_xor(meta[0], g))

    any_spec = pl.BlockSpec(memory_space=pl.ANY)
    in_specs = [any_spec] * len(pieces) + [
        pl.BlockSpec((1, width, chunk), opening),
        pl.BlockSpec((1, width, chunk), opening),
        pl.BlockSpec((exp_dev * units, slim), closing),
    ]
    operands = [*pieces, gate, up, down.reshape(exp_dev * units, width)]
    scratch = [
        pltpu.VMEM(shape, jnp.bfloat16),
        pltpu.VMEM((steps, rows, chunk), jnp.bfloat16),
        pltpu.VMEM((exp_dev, rows, LANES), jnp.float32),
        pltpu.SemaphoreType.DMA((len(pieces),)),
    ]
    if shared:
        gate_sh, up_sh, down_sh = shared
        units_sh = gate_sh.shape[1]
        in_specs += [
            pl.BlockSpec((width, units_sh), lambda i, meta: (0, 0)),
            pl.BlockSpec((width, units_sh), lambda i, meta: (0, 0)),
            pl.BlockSpec((units_sh, slim), closing),
        ]
        operands += [gate_sh, up_sh, down_sh]
        scratch.append(pltpu.VMEM((parts * part, units_sh), jnp.bfloat16))
    half = tp // 2

    def sending(i, meta):
        return (jnp.clip(i - steps, 0, half - 1), 0, 0)

    def keeping(i, meta):
        return (jnp.clip(i - steps - half, 0, half - 1), 0, 0)

    out = jax.ShapeDtypeStruct((half, rows, slim), jnp.bfloat16)
    return pl.pallas_call(
        functools.partial(
            expert_kernel, tuple(places), steps, exp_dev, experts, bool(shared), half
        ),
        grid_spec=pltpu.PrefetchScalarGridSpec(
            num_scalar_prefetch=1,
            grid=(steps + tp,),
            in_specs=in_specs,
            out_specs=(
                pl.BlockSpec((1, rows, slim), sending),
                pl.BlockSpec((1, rows, slim), keeping),
            ),
            scratch_shapes=scratch,
        ),
        out_shape=(out, out),
        compiler_params=pltpu.CompilerParams(dimension_semantics=("arbitrary",)),
        cost_estimate=pl.CostEstimate(
            flops=6 * rows * width * units * exp_dev,
            bytes_accessed=6 * width * units * exp_dev,
            transcendentals=rows * units * exp_dev,
        ),
        name=name,
    )(meta, *operands)


def add_up(*parts):
    total = parts[0].astype(jnp.float32)
    for part in parts[1:]:
        total = total + part.astype(jnp.float32)
    return total.astype(jnp.bfloat16)


def local(
    tokens_first,
    attn_gain,
    w_query,
    key_matrix,
    value_matrix,
    head_sink_logit,
    w_output,
    tokens_second,
    ffn_gain,
    routes,
    route_weight,
    w_gate_exp,
    w_up_exp,
    w_down_exp,
    w_gate_shared,
    w_up_shared,
    w_down_shared,
):
    rows_first = tokens_first.shape[0]
    norm_input = rms_scale(tokens_first, attn_gain)
    offset = lax.axis_index("ep") * rows_first
    token_positions = (offset + jnp.arange(rows_first, dtype=jnp.int32)).astype(jnp.float32)
    head_count = w_query.shape[1] // HEAD_SIZE
    key_heads = key_matrix.shape[1] // HEAD_SIZE
    head_group = head_count // key_heads
    query_rows = apply_rotary(
        jnp.dot(norm_input, w_query, preferred_element_type=jnp.float32).reshape(
            rows_first, head_count, HEAD_SIZE
        ),
        token_positions,
    ).astype(jnp.bfloat16)
    keys_local = apply_rotary(
        jnp.dot(norm_input, key_matrix, preferred_element_type=jnp.float32).reshape(
            rows_first, key_heads, HEAD_SIZE
        ),
        token_positions,
    ).astype(jnp.bfloat16)
    values_local = (
        jnp.dot(norm_input, value_matrix, preferred_element_type=jnp.float32)
        .astype(jnp.bfloat16)
        .reshape(rows_first, key_heads, HEAD_SIZE)
    )
    before = from_behind(
        jnp.concatenate(
            [keys_local[rows_first - BAND_LENGTH :], values_local[rows_first - BAND_LENGTH :]], axis=1
        ),
        "ep",
        1,
    )
    keys_before, values_before = before[:, :key_heads], before[:, key_heads:]
    keys_all = jnp.concatenate([keys_before, keys_local], axis=0)
    values_all = jnp.concatenate([values_before, values_local], axis=0)
    layer_block = min(512, rows_first)
    sink_scores = head_sink_logit.reshape(key_heads, head_group)[:, :, None, None]

    def attend(index):
        leading_row = index * layer_block
        block_queries = query_rows.reshape(layer_block, key_heads, head_group, HEAD_SIZE)
        scores = jnp.einsum(
            "qhgd,khd->hgqk", block_queries, keys_all, preferred_element_type=jnp.float32
        ) * HEAD_SIZE ** (-0.5)
        query_pos = offset + leading_row + jnp.arange(layer_block, dtype=jnp.int32)
        key_pos = (
            offset
            + leading_row
            - BAND_LENGTH
            + jnp.arange(layer_block + BAND_LENGTH, dtype=jnp.int32)
        )
        offsets = query_pos[:, None] - key_pos[None, :]
        visible = (offsets >= 0) & (offsets < BAND_LENGTH) & (key_pos[None, :] >= 0)
        scores = jnp.where(visible[None, None], scores, -jnp.inf)
        peak = jnp.maximum(jnp.max(scores, axis=-1, keepdims=True), sink_scores)
        expo = jnp.exp(scores - peak)
        total = jnp.sum(expo, axis=-1, keepdims=True) + jnp.exp(sink_scores - peak)
        weights = (expo / total).astype(jnp.bfloat16)
        mixed = jnp.einsum(
            "hgqk,khd->qhgd", weights, values_all, preferred_element_type=jnp.float32
        )
        return mixed.astype(jnp.bfloat16).reshape(layer_block, head_count * HEAD_SIZE)

    attended = lax.map(attend, jnp.arange(rows_first // layer_block, dtype=jnp.int32)).reshape(
        rows_first, head_count * HEAD_SIZE
    )
    tp = lax.axis_size("tp")
    index = lax.axis_index("tp")
    count = rows_first // tp

    def project(g):
        mine = lax.dynamic_slice_in_dim(attended, (index ^ g) * count, count, 0)
        return jnp.dot(mine, w_output, preferred_element_type=jnp.float32).astype(jnp.bfloat16)

    outward = swap(jnp.stack([project(g) for g in range(1, tp, 2)]), 0, 1)
    summed = [add_up(project(g), outward[g // 2]) for g in range(0, tp, 2)]
    mixer_out = add_up(
        summed[0], *[swap(summed[s], 0, s << 1) for s in range(1, tp // 2)]
    )
    ep, tp = lax.axis_size("ep"), lax.axis_size("tp")
    columns, lines = ep // 2, tp // 2
    index = lax.axis_index("tp").astype(jnp.int32)
    exp_dev = w_gate_exp.shape[0]
    experts = exp_dev * ep
    rows_second = tokens_second.shape[0]
    meta = jnp.stack([index, lax.axis_index("ep").astype(jnp.int32) * exp_dev])
    whole, half, quarter = pack(meta, tokens_second, ffn_gain, routes, route_weight, experts)
    total = whole.shape[1]
    cut = total // LANES // 2 * LANES
    beside = swap(half, 1, 0)
    along = jnp.stack([swap(quarter, s << 1, 0) for s in range(1, columns)])
    across = swap(along, 1, 0)
    rest_along, rest_across = [(along, 0, None)], [(across, 0, None)]
    for s in range(1, lines):
        other = swap(along, 0, s << 1)
        rest_along.append((other, s << 1, None))
        rest_across.append((swap(other[:, :, :cut], 1, 0), s << 1, (0, cut)))
        rest_across.append((swap(across[:, :, cut:], 0, s << 1), s << 1, (cut, total)))

    def with_core(listed):
        both = [(v, x, c or (0, total)) for v, x, c in listed]
        both += [(swap(v, 0, 1), x ^ 1, c) for v, x, c in both]
        return [v for v, _, _ in both], [(x, c) for _, x, c in both]

    send, keep = [], []
    shared = (w_gate_shared, w_up_shared, w_down_shared)
    near = ([whole.reshape(2, rows_second // 2, total), beside, swap(beside, 0, 1)],
            [(None, None), (0, None), (1, None)])
    shape_near = (2, 2, rows_second // 2, total)
    shape_far = (columns - 1, tp, rows_second // tp, total)
    for name, (pieces, places), shape, extra in (
        ("near", near, shape_near, shared),
        ("along", with_core(rest_along), shape_far, ()),
        ("across", with_core(rest_across), shape_far, ()),
    ):
        s, k = experts_call(meta, pieces, places, shape, w_gate_exp, w_up_exp, w_down_exp, extra, experts, name)
        blocks = shape[0]
        slim = s.shape[-1]
        sent = swap(s, 0, 1).reshape(lines, blocks, rows_second, slim)
        kept = k.reshape(lines, blocks, rows_second, slim)
        if lines == 1:
            keep.append(add_up(sent[0], kept[0]))
            continue
        out = [swap(add_up(sent[i], kept[i]), 0, i << 1) for i in range(1, lines)]
        keep.append(add_up(sent[0], kept[0], *out))
    near, along, across = keep
    far = swap(across, 1, 0)
    beside = swap(near[1], 1, 0)
    outgoing = add_up(along, far)
    arrived = [swap(outgoing[s - 1], s << 1, 0) for s in range(1, columns)]
    moe_out = add_up(near[0], beside, *arrived)
    return (mixer_out, moe_out)


def solution(mesh):
    in_specs = (
        P("ep", None),
        P(),
        P(None, "tp"),
        P(None, "tp"),
        P(None, "tp"),
        P("tp"),
        P("tp", None),
        P("ep", None),
        P(),
        P("ep", None),
        P("ep", None),
        P("ep", None, "tp"),
        P("ep", None, "tp"),
        P("ep", "tp", None),
        P(None, "tp"),
        P(None, "tp"),
        P("tp", None),
    )
    out_specs = (P(("ep", "tp"), None), P("ep", "tp"))
    return jax.shard_map(local, mesh=mesh, in_specs=in_specs, out_specs=out_specs, check_vma=False)
```

```python
import functools

import jax
import jax.numpy as jnp
from jax import lax
from jax.experimental import pallas as pl
from jax.experimental.pallas import tpu as pltpu
from jax.sharding import PartitionSpec as P

HEAD_SIZE = 64
BAND_LENGTH = 128


rope_base = 10000.0
norm_eps = 1e-06


LANES = 128
SMEM = pl.BlockSpec(memory_space=pltpu.SMEM)
HBM = pl.BlockSpec(memory_space=pltpu.HBM)
VMEM = pl.BlockSpec(memory_space=pltpu.VMEM)


def swap(value, ep_bits, tp_bits):
    ep, tp = lax.axis_size("ep"), lax.axis_size("tp")
    pairs = [
        (e * tp + t, (e ^ ep_bits) * tp + (t ^ tp_bits)) for e in range(ep) for t in range(tp)
    ]
    return lax.ppermute(value, ("ep", "tp"), pairs)


def limit(mib):
    return pltpu.CompilerParams(vmem_limit_bytes=mib << 20)


def in_hbm(*values):
    return [pltpu.with_memory_space_constraint(value, pltpu.HBM) for value in values]


def load(pairs, sems):
    copies = [pltpu.make_async_copy(a, b, sems.at[i]) for i, (a, b) in enumerate(pairs)]
    for copy in copies:
        copy.start()
    return copies


def turn(values, cosine, sine):
    width = values.shape[1]
    half = HEAD_SIZE // 2
    lane = lax.broadcasted_iota(jnp.int32, values.shape, 1)
    upper = pltpu.roll(values, half, 1)
    lower = pltpu.roll(values, width - half, 1)
    other = jnp.where(lane % HEAD_SIZE < half, -lower, upper)
    repeat = width // LANES
    if repeat > 1:
        cosine = jnp.concatenate([cosine] * repeat, axis=1)
        sine = jnp.concatenate([sine] * repeat, axis=1)
    return values * cosine + other * sine


def project_kernel(*refs):
    sources, (cosine, sine), (queries, pairs, last) = refs[:5], refs[5:7], refs[7:10]
    (tokens, gain, query_w, key_w, value_w), sems = refs[10:15], refs[15]
    rows = tokens.shape[0]
    step = min(128, rows)
    parts = [slice(low, low + step) for low in range(0, rows, step)]
    first = [(sources[1], gain)] + [(sources[0].at[p, :], tokens.at[p, :]) for p in parts[:1]]
    rest = [(sources[i], refs[10 + i]) for i in (2, 3, 4)]
    rest += [(sources[0].at[p, :], tokens.at[p, :]) for p in parts[1:]]
    copies = load(first + rest, sems)
    for number, part in enumerate(parts):
        for copy in copies[:2] if number == 0 else copies[4 + number : 5 + number]:
            copy.wait()
        wide = tokens[part, :].astype(jnp.float32)
        scaled = wide * lax.rsqrt(jnp.mean(wide * wide, axis=-1, keepdims=True) + norm_eps)
        normed = (scaled * gain[...]).astype(jnp.bfloat16)
        if number == 0:
            for copy in copies[2:5]:
                copy.wait()
        query = jnp.dot(normed, query_w[...], preferred_element_type=jnp.float32)
        turned = turn(query, cosine[part, :], sine[part, :])
        queries[part, :] = turned.astype(jnp.bfloat16) * jnp.bfloat16(HEAD_SIZE ** (-0.5))
        key = jnp.dot(normed, key_w[...], preferred_element_type=jnp.float32)
        value = jnp.dot(normed, value_w[...], preferred_element_type=jnp.float32)
        both = jnp.concatenate([key, value], axis=1)
        lane = lax.broadcasted_iota(jnp.int32, both.shape, 1)
        turned = turn(both, cosine[part, :], sine[part, :])
        pairs[part, :] = jnp.where(lane < key.shape[1], turned, both).astype(jnp.bfloat16)
    last[...] = pairs[rows - BAND_LENGTH :, :]


def attend_kernel(
    meta, sinks, queries, pairs, before, source, send, keep, attended, output_w, sems
):
    (copy,) = load([(source, output_w)], sems)
    rows, q_width = queries.shape
    width = pairs.shape[1] // 2
    groups = q_width // width
    band = BAND_LENGTH
    place = lax.broadcasted_iota(jnp.int32, (band, 2 * band), 0)
    other = lax.broadcasted_iota(jnp.int32, (band, 2 * band), 1)
    within = (other > place) & (other <= place + band)
    first = within & (other >= jnp.where(meta[2] == 0, band, 0))
    for low in range(0, rows, band):
        visible = first if low == 0 else within
        visible = jnp.concatenate([visible] * groups, axis=0)
        if low == 0:
            window = jnp.concatenate([before[...], pairs[:band, :]], axis=0)
        else:
            window = pairs[low - band : low + band, :]
        out = []
        for h in range(width // HEAD_SIZE):
            keys = window[:, h * HEAD_SIZE : (h + 1) * HEAD_SIZE]
            values = window[:, width + h * HEAD_SIZE : width + (h + 1) * HEAD_SIZE]
            heads = range(h * groups, (h + 1) * groups)
            asked = jnp.concatenate(
                [queries[low : low + band, i * HEAD_SIZE : (i + 1) * HEAD_SIZE] for i in heads], axis=0
            )
            score = lax.dot_general(
                asked, keys, (((1,), (1,)), ((), ())), preferred_element_type=jnp.float32
            )
            score = jnp.where(visible, score, -jnp.inf)
            sink = jnp.concatenate([jnp.full((band, 1), sinks[i], jnp.float32) for i in heads], axis=0)
            peak = jnp.maximum(jnp.max(score, axis=1, keepdims=True), sink)
            expo = jnp.exp(score - peak)
            whole = jnp.sum(expo, axis=1, keepdims=True) + jnp.exp(sink - peak)
            weight = (expo * (1.0 / whole)).astype(jnp.bfloat16)
            mixed = jnp.dot(weight, values, preferred_element_type=jnp.float32)
            out += [mixed[i * band : (i + 1) * band] for i in range(groups)]
        attended[low : low + band, :] = jnp.concatenate(out, axis=1).astype(jnp.bfloat16)
    half, count, _ = send.shape
    copy.wait()
    for k in range(2 * half):
        out, g = (send, 2 * k + 1) if k < half else (keep, 2 * (k - half))
        start = pl.multiple_of((meta[0] ^ g) * count, count)
        out[k % half] = jnp.dot(
            attended[pl.ds(start, count), :], output_w[...], preferred_element_type=jnp.float32
        ).astype(jnp.bfloat16)


def pack_kernel(experts, tp, meta, *refs):
    sources, (whole, half, quarter), held, sems = refs[:4], refs[4:7], refs[7:11], refs[11]
    for copy in load(list(zip(sources, held)), sems):
        copy.wait()
    tokens, gain, routes, weight = held
    rows, width = tokens.shape
    wide = tokens[...].astype(jnp.float32)
    scaled = wide * lax.rsqrt(jnp.mean(wide * wide, axis=-1, keepdims=True) + norm_eps)
    whole[:, :width] = (scaled * gain[...]).astype(jnp.bfloat16)
    pad = whole.shape[1] - width
    line = lax.broadcasted_iota(jnp.int32, (pad, rows), 0)
    named = jnp.where(line < experts, line, line - experts)
    dense = jnp.zeros((pad, rows), jnp.float32)
    for k in range(routes.shape[0]):
        dense = dense + jnp.where(named == routes[k : k + 1, :], weight[k : k + 1, :], 0.0)
    high = dense.astype(jnp.bfloat16).astype(jnp.float32)
    cols = jnp.where(line < experts, high, jnp.where(line < 2 * experts, dense - high, 0.0))
    whole[:, width:] = cols.T.astype(jnp.bfloat16)
    part = rows // 2
    half[...] = whole[pl.ds(pl.multiple_of((meta[0] % 2) * part, part), part), :]
    part = rows // tp
    quarter[...] = whole[pl.ds(pl.multiple_of(meta[0] * part, part), part), :]


def pack(meta, tokens, gain, routes, weight, experts):
    rows, width = tokens.shape
    tp = lax.axis_size("tp")
    total = width + -(-2 * experts // LANES) * LANES
    return pl.pallas_call(
        functools.partial(pack_kernel, experts, tp),
        out_shape=tuple(
            jax.ShapeDtypeStruct((n, total), jnp.bfloat16) for n in (rows, rows // 2, rows // tp)
        ),
        in_specs=[SMEM] + [HBM] * 4,
        out_specs=(VMEM,) * 3,
        scratch_shapes=[
            pltpu.VMEM((rows, width), jnp.bfloat16),
            pltpu.VMEM((1, width), jnp.float32),
            pltpu.VMEM(routes.shape[::-1], jnp.int32),
            pltpu.VMEM(weight.shape[::-1], jnp.float32),
            pltpu.SemaphoreType.DMA((4,)),
        ],
        cost_estimate=pl.CostEstimate(flops=1 << 26, bytes_accessed=1 << 20, transcendentals=0),
        compiler_params=limit(8),
        name="pack",
    )(meta, *in_hbm(tokens, gain.reshape(1, -1), routes.T, weight.T))


def join_kernel(*refs):
    for i, ref in enumerate(refs[:-1]):
        refs[-1][i] = ref[...]


def join(parts):
    return pl.pallas_call(
        join_kernel,
        out_shape=jax.ShapeDtypeStruct((len(parts), *parts[0].shape), parts[0].dtype),
        in_specs=[VMEM] * len(parts),
        out_specs=VMEM,
        cost_estimate=pl.CostEstimate(flops=1 << 20, bytes_accessed=1 << 20, transcendentals=0),
        compiler_params=limit(8),
        name="join",
    )(*parts)


def silu(v):
    return v / (1.0 + jnp.exp(-v))


def expert_kernel(places, blocks, experts, shared, meta, *refs):
    pieces, refs = refs[: len(places)], refs[len(places) :]
    weights, refs = refs[: 6 if shared else 3], refs[6 if shared else 3 :]
    send, keep, held, hidden = refs[:4]
    stored, sems = refs[4:-1], refs[-1]
    gate, up, down = stored[:3]
    exp_dev, width, units = gate.shape
    half, rows, slim = send.shape
    size = rows // blocks
    chunk = min(256, units)
    order = [(2 * k + 1 if k < half else 2 * (k - half)) for k in range(2 * half)]
    starts = [pl.multiple_of((meta[0] ^ g) * slim, slim) for g in order]
    copies = {}

    def fetch(key, number, part):
        copies[key] = pltpu.make_async_copy(
            weights[number].at[part], stored[number].at[part], sems.at[len(copies)]
        )
        copies[key].start()

    whole = (slice(None), slice(None))
    for j in range(exp_dev):
        for c in range(0, units, chunk):
            for number in (0, 1):
                fetch((number, j, c), number, (j, slice(None), slice(c, c + chunk)))
    if shared:
        fetch("gate", 3, whole)
        fetch("up", 4, whole)
        fetch("down", 5, whole)
    for k in range(2 * half):
        fetch((2, k), 2, (slice(None), pl.ds(starts[k], slim)))

    for piece, (first, xor, number) in zip(pieces, places):
        part = piece.shape[1]
        where = 0 if xor is None else (meta[0] % number) ^ xor
        for b in range(piece.shape[0]):
            start = pl.multiple_of((first + b) * size + where * part, part)
            held[pl.ds(start, part), :] = piece[b]
    several = max(n for n in (1, 2, 3) if blocks % n == 0)
    most = several * size

    def over_rows(body):
        if most == rows:
            body(pl.ds(0, rows))
        else:

            @pl.loop(0, rows // most)
            def _(i):
                body(pl.ds(pl.multiple_of(i * most, most), most))

    def scale(at, j):
        cols = held[at, width:].astype(jnp.float32)
        lane = lax.broadcasted_iota(jnp.int32, cols.shape, 1)
        mine = meta[1] + j
        chosen = (lane == mine) | (lane == mine + experts)
        return jnp.sum(jnp.where(chosen, cols, 0.0), axis=1, keepdims=True)

    for j in range(exp_dev):
        for c in range(0, units, chunk):
            copies[0, j, c].wait()
            copies[1, j, c].wait()

            def opening(at, j=j, c=c):
                tokens = held[at, :width]
                opened = jnp.dot(tokens, gate[j, :, c : c + chunk], preferred_element_type=jnp.float32)
                lifted = jnp.dot(tokens, up[j, :, c : c + chunk], preferred_element_type=jnp.float32)
                hidden[at, j * units + c : j * units + c + chunk] = (
                    silu(opened) * lifted * scale(at, j)
                ).astype(jnp.bfloat16)

            over_rows(opening)
    if shared:
        copies["gate"].wait()
        copies["up"].wait()
        own = held[:size, :width]
        hidden_sh = (
            silu(jnp.dot(own, stored[3][...], preferred_element_type=jnp.float32))
            * jnp.dot(own, stored[4][...], preferred_element_type=jnp.float32)
        ).astype(jnp.bfloat16)
        copies["down"].wait()
    for k in range(2 * half):
        out = send if k < half else keep
        copies[2, k].wait()

        def closing(at, k=k, out=out):
            result = jnp.dot(
                hidden[at, :], down[:, pl.ds(starts[k], slim)], preferred_element_type=jnp.float32
            )
            if shared:
                extra = jnp.dot(
                    hidden_sh, stored[5][:, pl.ds(starts[k], slim)], preferred_element_type=jnp.float32
                )
                out[k % half, :size, :] = (result[:size] + extra).astype(jnp.bfloat16)
                out[k % half, size:, :] = result[size:].astype(jnp.bfloat16)
            else:
                out[k % half, at, :] = result.astype(jnp.bfloat16)

        over_rows(closing)


def experts_call(meta, pieces, places, blocks, size, gate, up, down, shared, experts):
    exp_dev, width, units = gate.shape
    tp = lax.axis_size("tp")
    rows = blocks * size
    total = pieces[0].shape[-1]
    weights = [gate, up, down.reshape(exp_dev * units, width), *shared]
    out = jax.ShapeDtypeStruct((tp // 2, rows, width // tp), jnp.bfloat16)
    copies = 2 * exp_dev * (units // min(256, units)) + tp + len(shared)
    return pl.pallas_call(
        functools.partial(expert_kernel, tuple(places), blocks, experts, bool(shared)),
        in_specs=[SMEM] + [VMEM] * len(pieces) + [HBM] * len(weights),
        out_specs=(VMEM, VMEM),
        scratch_shapes=[
            pltpu.VMEM((rows, total), jnp.bfloat16),
            pltpu.VMEM((rows, exp_dev * units), jnp.bfloat16),
            *[pltpu.VMEM(w.shape, w.dtype) for w in weights],
            pltpu.SemaphoreType.DMA((copies,)),
        ],
        out_shape=(out, out),
        cost_estimate=pl.CostEstimate(
            flops=6 * rows * width * units * exp_dev,
            bytes_accessed=6 * width * units * exp_dev,
            transcendentals=rows * units * exp_dev,
        ),
        compiler_params=limit(36),
    )(meta, *pieces, *in_hbm(*weights))


def add_up(*parts):
    total = parts[0].astype(jnp.float32)
    for part in parts[1:]:
        total = total + part.astype(jnp.float32)
    return total.astype(jnp.bfloat16)


def local(
    tokens_first,
    attn_gain,
    w_query,
    key_matrix,
    value_matrix,
    head_sink_logit,
    w_output,
    tokens_second,
    ffn_gain,
    routes,
    route_weight,
    w_gate_exp,
    w_up_exp,
    w_down_exp,
    w_gate_shared,
    w_up_shared,
    w_down_shared,
):
    ep, tp = lax.axis_size("ep"), lax.axis_size("tp")
    index = lax.axis_index("tp").astype(jnp.int32)
    exp_dev = w_gate_exp.shape[0]
    experts = exp_dev * ep
    turn_ep = lax.axis_index("ep").astype(jnp.int32)
    meta = jnp.stack([index, turn_ep * exp_dev, turn_ep])
    columns, lines = ep // 2, tp // 2
    rows_second = tokens_second.shape[0]
    whole, half, quarter = pack(meta, tokens_second, ffn_gain, routes, route_weight, experts)
    beside = swap(half, 1, 0)[None]
    around = [swap(quarter, s << 1, 0) for s in range(1, columns)]

    rows_first = tokens_first.shape[0]
    offset = lax.axis_index("ep") * rows_first
    token_positions = (offset + jnp.arange(rows_first, dtype=jnp.int32)).astype(jnp.float32)
    freqs = rope_base ** (-jnp.arange(0, HEAD_SIZE, 2, dtype=jnp.float32) / HEAD_SIZE)
    angles = token_positions[:, None] * jnp.tile(freqs, 2 * LANES // HEAD_SIZE)[None, :]
    wide_kv = key_matrix.shape[1] + value_matrix.shape[1]
    queries, pairs, last = pl.pallas_call(
        project_kernel,
        out_shape=(
            jax.ShapeDtypeStruct((rows_first, w_query.shape[1]), jnp.bfloat16),
            jax.ShapeDtypeStruct((rows_first, wide_kv), jnp.bfloat16),
            jax.ShapeDtypeStruct((BAND_LENGTH, wide_kv), jnp.bfloat16),
        ),
        in_specs=[HBM] * 5 + [VMEM] * 2,
        out_specs=(VMEM,) * 3,
        scratch_shapes=[
            pltpu.VMEM(tokens_first.shape, jnp.bfloat16),
            pltpu.VMEM((1, attn_gain.shape[0]), jnp.float32),
            pltpu.VMEM(w_query.shape, jnp.bfloat16),
            pltpu.VMEM(key_matrix.shape, jnp.bfloat16),
            pltpu.VMEM(value_matrix.shape, jnp.bfloat16),
            pltpu.SemaphoreType.DMA((4 + rows_first // min(128, rows_first),)),
        ],
        cost_estimate=pl.CostEstimate(flops=1 << 30, bytes_accessed=1 << 22, transcendentals=0),
        compiler_params=limit(24),
        name="project",
    )(
        *in_hbm(tokens_first, attn_gain.reshape(1, -1), w_query, key_matrix, value_matrix),
        jnp.cos(angles), jnp.sin(angles),
    )
    before = lax.ppermute(last, "ep", [(i, i + 1) for i in range(ep - 1)])
    count = rows_first // tp
    part = jax.ShapeDtypeStruct((lines, count, w_output.shape[1]), jnp.bfloat16)
    outward, kept = pl.pallas_call(
        attend_kernel,
        out_shape=(part, part),
        in_specs=[SMEM] * 2 + [VMEM] * 3 + [HBM],
        out_specs=(VMEM,) * 2,
        scratch_shapes=[
            pltpu.VMEM((rows_first, w_query.shape[1]), jnp.bfloat16),
            pltpu.VMEM(w_output.shape, jnp.bfloat16),
            pltpu.SemaphoreType.DMA((1,)),
        ],
        cost_estimate=pl.CostEstimate(flops=1 << 30, bytes_accessed=1 << 22, transcendentals=0),
        compiler_params=limit(24),
        name="attend",
    )(meta, head_sink_logit, queries, pairs, before, *in_hbm(w_output))
    outward = swap(outward, 0, 1)
    mixer_out = add_up(
        outward[0],
        kept[0],
        *[swap(add_up(outward[s], kept[s]), 0, s << 1) for s in range(1, lines)],
    )
    along = join(around)
    across = swap(along, 1, 0)
    rest_along, rest_across = [(along, 0)], [(across, 0)]
    for s in range(1, lines):
        other = swap(along, 0, s << 1)
        rest_along.append((other, s << 1))
        rest_across.append((swap(other, 1, 0), s << 1))

    def with_core(listed):
        listed = listed + [(swap(v, 0, 1), x ^ 1) for v, x in listed]
        return [v for v, _ in listed], [(0, x, tp) for _, x in listed]

    near = ([whole[None], beside, swap(beside, 0, 1)], [(0, None, 1), (1, 0, 2), (1, 1, 2)])
    shared = (w_gate_shared, w_up_shared, w_down_shared)
    keep = []
    for name, (pieces, places), blocks, extra in (
        ("near", near, 2, shared),
        ("along", with_core(rest_along), columns - 1, ()),
        ("across", with_core(rest_across), columns - 1, ()),
    ):
        s, k = experts_call(
            meta, pieces, places, blocks, rows_second,
            w_gate_exp, w_up_exp, w_down_exp, extra, experts,
        )
        slim = s.shape[-1]
        sent = swap(s, 0, 1).reshape(lines, blocks, rows_second, slim)
        kept = k.reshape(lines, blocks, rows_second, slim)
        gone = [add_up(sent[i], kept[i]) for i in range(1, lines)]
        if gone and name != "near":
            meta, *gone = lax.optimization_barrier((meta, *gone))
        out = [swap(gone[i - 1], 0, i << 1) for i in range(1, lines)]
        keep.append(add_up(sent[0], kept[0], *out))
    near, along, across = keep
    far = swap(across, 1, 0)
    beside = swap(near[1], 1, 0)
    outgoing = add_up(along, far)
    arrived = [swap(outgoing[s - 1], s << 1, 0) for s in range(1, columns)]
    moe_out = add_up(near[0], beside, *arrived)
    return (mixer_out, moe_out)


def solution(mesh):
    in_specs = (
        P("ep", None),
        P(),
        P(None, "tp"),
        P(None, "tp"),
        P(None, "tp"),
        P("tp"),
        P("tp", None),
        P("ep", None),
        P(),
        P("ep", None),
        P("ep", None),
        P("ep", None, "tp"),
        P("ep", None, "tp"),
        P("ep", "tp", None),
        P(None, "tp"),
        P(None, "tp"),
        P("tp", None),
    )
    out_specs = (P(("ep", "tp"), None), P("ep", "tp"))

    return jax.shard_map(local, mesh=mesh, in_specs=in_specs, out_specs=out_specs, check_vma=False)
```

```python
import functools

import jax
import jax.numpy as jnp
from jax import lax
from jax.experimental import pallas as pl
from jax.experimental.pallas import tpu as pltpu
from jax.sharding import PartitionSpec as P

HEAD_SIZE = 64
BAND_LENGTH = 128


rope_base = 10000.0
norm_eps = 1e-06


LANES = 128
SMEM = pl.BlockSpec(memory_space=pltpu.SMEM)
HBM = pl.BlockSpec(memory_space=pltpu.HBM)
VMEM = pl.BlockSpec(memory_space=pltpu.VMEM)


def swap(value, ep_bits, tp_bits):
    ep, tp = lax.axis_size("ep"), lax.axis_size("tp")
    pairs = [
        (e * tp + t, (e ^ ep_bits) * tp + (t ^ tp_bits)) for e in range(ep) for t in range(tp)
    ]
    return lax.ppermute(value, ("ep", "tp"), pairs)


def limit(mib):
    return pltpu.CompilerParams(vmem_limit_bytes=mib << 20)


def in_hbm(*values):
    return [pltpu.with_memory_space_constraint(value, pltpu.HBM) for value in values]


def in_vmem(*values):
    return [pltpu.with_memory_space_constraint(value, pltpu.VMEM) for value in values]


def load(pairs, sems):
    copies = [pltpu.make_async_copy(a, b, sems.at[i]) for i, (a, b) in enumerate(pairs)]
    for copy in copies:
        copy.start()
    return copies


def turn(values, cosine, sine):
    width = values.shape[1]
    half = HEAD_SIZE // 2
    lane = lax.broadcasted_iota(jnp.int32, values.shape, 1)
    upper = pltpu.roll(values, half, 1)
    lower = pltpu.roll(values, width - half, 1)
    other = jnp.where(lane % HEAD_SIZE < half, -lower, upper)
    repeat = width // LANES
    if repeat > 1:
        cosine = jnp.concatenate([cosine] * repeat, axis=1)
        sine = jnp.concatenate([sine] * repeat, axis=1)
    return values * cosine + other * sine


def project_kernel(*refs):
    sources, (cosine, sine), (queries, pairs, last) = refs[:5], refs[5:7], refs[7:10]
    (tokens, gain, query_w, key_w, value_w), sems = refs[10:15], refs[15]
    rows = tokens.shape[0]
    step = min(128, rows)
    parts = [slice(low, low + step) for low in range(0, rows, step)]
    first = [(sources[1], gain)] + [(sources[0].at[p, :], tokens.at[p, :]) for p in parts[:1]]
    rest = [(sources[i], refs[10 + i]) for i in (2, 3, 4)]
    rest += [(sources[0].at[p, :], tokens.at[p, :]) for p in parts[1:]]
    copies = load(first + rest, sems)
    for number, part in enumerate(parts):
        for copy in copies[:2] if number == 0 else copies[4 + number : 5 + number]:
            copy.wait()
        wide = tokens[part, :].astype(jnp.float32)
        scaled = wide * lax.rsqrt(jnp.mean(wide * wide, axis=-1, keepdims=True) + norm_eps)
        normed = (scaled * gain[...]).astype(jnp.bfloat16)
        if number == 0:
            for copy in copies[2:5]:
                copy.wait()
        query = jnp.dot(normed, query_w[...], preferred_element_type=jnp.float32)
        turned = turn(query, cosine[part, :], sine[part, :])
        queries[part, :] = turned.astype(jnp.bfloat16) * jnp.bfloat16(HEAD_SIZE ** (-0.5))
        key = jnp.dot(normed, key_w[...], preferred_element_type=jnp.float32)
        value = jnp.dot(normed, value_w[...], preferred_element_type=jnp.float32)
        both = jnp.concatenate([key, value], axis=1)
        lane = lax.broadcasted_iota(jnp.int32, both.shape, 1)
        turned = turn(both, cosine[part, :], sine[part, :])
        pairs[part, :] = jnp.where(lane < key.shape[1], turned, both).astype(jnp.bfloat16)
    last[...] = pairs[rows - BAND_LENGTH :, :]


def attend_kernel(ahead, meta, sinks, queries, pairs, before, source, *refs):
    (send, keep), (attended, output_w, sems) = refs[ahead : ahead + 2], refs[2 * ahead + 2 :]
    copy, *early = load(
        [(source, output_w), *zip(refs[:ahead], refs[ahead + 2 : 2 * ahead + 2])], sems
    )
    rows, q_width = queries.shape
    width = pairs.shape[1] // 2
    groups = q_width // width
    band = BAND_LENGTH
    place = lax.broadcasted_iota(jnp.int32, (band, 2 * band), 0)
    other = lax.broadcasted_iota(jnp.int32, (band, 2 * band), 1)
    within = (other > place) & (other <= place + band)
    first = within & (other >= jnp.where(meta[2] == 0, band, 0))
    for low in range(0, rows, band):
        visible = first if low == 0 else within
        visible = jnp.concatenate([visible] * groups, axis=0)
        if low == 0:
            window = jnp.concatenate([before[...], pairs[:band, :]], axis=0)
        else:
            window = pairs[low - band : low + band, :]
        out = []
        for h in range(width // HEAD_SIZE):
            keys = window[:, h * HEAD_SIZE : (h + 1) * HEAD_SIZE]
            values = window[:, width + h * HEAD_SIZE : width + (h + 1) * HEAD_SIZE]
            heads = range(h * groups, (h + 1) * groups)
            asked = jnp.concatenate(
                [queries[low : low + band, i * HEAD_SIZE : (i + 1) * HEAD_SIZE] for i in heads], axis=0
            )
            score = lax.dot_general(
                asked, keys, (((1,), (1,)), ((), ())), preferred_element_type=jnp.float32
            )
            score = jnp.where(visible, score, -jnp.inf)
            sink = jnp.concatenate([jnp.full((band, 1), sinks[i], jnp.float32) for i in heads], axis=0)
            peak = jnp.maximum(jnp.max(score, axis=1, keepdims=True), sink)
            expo = jnp.exp(score - peak)
            whole = jnp.sum(expo, axis=1, keepdims=True) + jnp.exp(sink - peak)
            weight = (expo * (1.0 / whole)).astype(jnp.bfloat16)
            mixed = jnp.dot(weight, values, preferred_element_type=jnp.float32)
            out += [mixed[i * band : (i + 1) * band] for i in range(groups)]
        attended[low : low + band, :] = jnp.concatenate(out, axis=1).astype(jnp.bfloat16)
    half, count, _ = send.shape
    copy.wait()
    for k in range(2 * half):
        out, g = (send, 2 * k + 1) if k < half else (keep, 2 * (k - half))
        start = pl.multiple_of((meta[0] ^ g) * count, count)
        out[k % half] = jnp.dot(
            attended[pl.ds(start, count), :], output_w[...], preferred_element_type=jnp.float32
        ).astype(jnp.bfloat16)
    for copy in early:
        copy.wait()


def pack_kernel(experts, tp, meta, *refs):
    sources, (whole, half, quarter), held, sems = refs[:4], refs[4:7], refs[7:11], refs[11]
    for copy in load(list(zip(sources, held)), sems):
        copy.wait()
    tokens, gain, routes, weight = held
    rows, width = tokens.shape
    wide = tokens[...].astype(jnp.float32)
    scaled = wide * lax.rsqrt(jnp.mean(wide * wide, axis=-1, keepdims=True) + norm_eps)
    whole[:, :width] = (scaled * gain[...]).astype(jnp.bfloat16)
    pad = whole.shape[1] - width
    line = lax.broadcasted_iota(jnp.int32, (pad, rows), 0)
    named = jnp.where(line < experts, line, line - experts)
    dense = jnp.zeros((pad, rows), jnp.float32)
    for k in range(routes.shape[0]):
        dense = dense + jnp.where(named == routes[k : k + 1, :], weight[k : k + 1, :], 0.0)
    high = dense.astype(jnp.bfloat16).astype(jnp.float32)
    cols = jnp.where(line < experts, high, jnp.where(line < 2 * experts, dense - high, 0.0))
    whole[:, width:] = cols.T.astype(jnp.bfloat16)
    part = rows // 2
    half[...] = whole[pl.ds(pl.multiple_of((meta[0] % 2) * part, part), part), :]
    part = rows // tp
    quarter[...] = whole[pl.ds(pl.multiple_of(meta[0] * part, part), part), :]


def pack(meta, tokens, gain, routes, weight, experts):
    rows, width = tokens.shape
    tp = lax.axis_size("tp")
    total = width + -(-2 * experts // LANES) * LANES
    return pl.pallas_call(
        functools.partial(pack_kernel, experts, tp),
        out_shape=tuple(
            jax.ShapeDtypeStruct((n, total), jnp.bfloat16) for n in (rows, rows // 2, rows // tp)
        ),
        in_specs=[SMEM] + [HBM] * 4,
        out_specs=(VMEM,) * 3,
        scratch_shapes=[
            pltpu.VMEM((rows, width), jnp.bfloat16),
            pltpu.VMEM((1, width), jnp.float32),
            pltpu.VMEM(routes.shape[::-1], jnp.int32),
            pltpu.VMEM(weight.shape[::-1], jnp.float32),
            pltpu.SemaphoreType.DMA((4,)),
        ],
        cost_estimate=pl.CostEstimate(flops=1 << 26, bytes_accessed=1 << 20, transcendentals=0),
        compiler_params=limit(8),
        name="pack",
    )(meta, *in_hbm(tokens, gain.reshape(1, -1), routes.T, weight.T))


def join_kernel(*refs):
    for i, ref in enumerate(refs[:-1]):
        refs[-1][i] = ref[...]


def join(parts):
    return pl.pallas_call(
        join_kernel,
        out_shape=jax.ShapeDtypeStruct((len(parts), *parts[0].shape), parts[0].dtype),
        in_specs=[VMEM] * len(parts),
        out_specs=VMEM,
        cost_estimate=pl.CostEstimate(flops=1 << 20, bytes_accessed=1 << 20, transcendentals=0),
        compiler_params=limit(8),
        name="join",
    )(*parts)


def silu(v):
    return v / (1.0 + jnp.exp(-v))


def expert_kernel(places, blocks, experts, shared, meta, *refs):
    pieces, refs = refs[: len(places)], refs[len(places) :]
    weights, refs = refs[: 6 if shared else 3], refs[6 if shared else 3 :]
    send, keep, held, hidden = refs
    gate, up, down = weights[:3]
    exp_dev, width, units = gate.shape
    half, rows, slim = send.shape
    size = rows // blocks
    chunk = min(256, units)
    order = [(2 * k + 1 if k < half else 2 * (k - half)) for k in range(2 * half)]
    starts = [pl.multiple_of((meta[0] ^ g) * slim, slim) for g in order]

    for piece, (first, xor, number, col) in zip(pieces, places):
        part = piece.shape[1]
        where = 0 if xor is None else (meta[0] % number) ^ xor
        for b in range(piece.shape[0]):
            start = pl.multiple_of((first + b) * size + where * part, part)
            held[pl.ds(start, part), col : col + piece.shape[2]] = piece[b]
    several = max(n for n in (1, 2, 3) if blocks % n == 0)
    most = several * size

    def over_rows(body):
        if most == rows:
            body(pl.ds(0, rows))
        else:

            @pl.loop(0, rows // most)
            def _(i):
                body(pl.ds(pl.multiple_of(i * most, most), most))

    def scale(at, j):
        cols = held[at, width:].astype(jnp.float32)
        lane = lax.broadcasted_iota(jnp.int32, cols.shape, 1)
        mine = meta[1] + j
        chosen = (lane == mine) | (lane == mine + experts)
        return jnp.sum(jnp.where(chosen, cols, 0.0), axis=1, keepdims=True)

    for j in range(exp_dev):
        for c in range(0, units, chunk):

            def opening(at, j=j, c=c):
                tokens = held[at, :width]
                opened = jnp.dot(tokens, gate[j, :, c : c + chunk], preferred_element_type=jnp.float32)
                lifted = jnp.dot(tokens, up[j, :, c : c + chunk], preferred_element_type=jnp.float32)
                hidden[at, j * units + c : j * units + c + chunk] = (
                    silu(opened) * lifted * scale(at, j)
                ).astype(jnp.bfloat16)

            over_rows(opening)
    if shared:
        own = held[:size, :width]
        hidden_sh = (
            silu(jnp.dot(own, weights[3][...], preferred_element_type=jnp.float32))
            * jnp.dot(own, weights[4][...], preferred_element_type=jnp.float32)
        ).astype(jnp.bfloat16)
    for k in range(2 * half):
        out = send if k < half else keep

        def closing(at, k=k, out=out):
            rows_down = [down[j, :, pl.ds(starts[k], slim)] for j in range(exp_dev)]
            result = jnp.dot(
                hidden[at, :], jnp.concatenate(rows_down, axis=0), preferred_element_type=jnp.float32
            )
            if shared:
                extra = jnp.dot(
                    hidden_sh, weights[5][:, pl.ds(starts[k], slim)], preferred_element_type=jnp.float32
                )
                out[k % half, :size, :] = (result[:size] + extra).astype(jnp.bfloat16)
                out[k % half, size:, :] = result[size:].astype(jnp.bfloat16)
            else:
                out[k % half, at, :] = result.astype(jnp.bfloat16)

        over_rows(closing)


def experts_call(meta, pieces, places, blocks, size, gate, up, down, shared, experts):
    exp_dev, width, units = gate.shape
    tp = lax.axis_size("tp")
    rows = blocks * size
    total = width + -(-2 * experts // LANES) * LANES
    weights = [gate, up, down, *shared]
    out = jax.ShapeDtypeStruct((tp // 2, rows, width // tp), jnp.bfloat16)
    return pl.pallas_call(
        functools.partial(expert_kernel, tuple(places), blocks, experts, bool(shared)),
        in_specs=[SMEM] + [VMEM] * (len(pieces) + len(weights)),
        out_specs=(VMEM, VMEM),
        scratch_shapes=[
            pltpu.VMEM((rows, total), jnp.bfloat16),
            pltpu.VMEM((rows, exp_dev * units), jnp.bfloat16),
        ],
        out_shape=(out, out),
        cost_estimate=pl.CostEstimate(
            flops=6 * rows * width * units * exp_dev,
            bytes_accessed=6 * width * units * exp_dev,
            transcendentals=rows * units * exp_dev,
        ),
        compiler_params=limit(14 + (8 * rows * total >> 20)),
    )(meta, *pieces, *in_vmem(*weights))


def add_up(*parts):
    total = parts[0].astype(jnp.float32)
    for part in parts[1:]:
        total = total + part.astype(jnp.float32)
    return total.astype(jnp.bfloat16)


def local(
    tokens_first,
    attn_gain,
    w_query,
    key_matrix,
    value_matrix,
    head_sink_logit,
    w_output,
    tokens_second,
    ffn_gain,
    routes,
    route_weight,
    w_gate_exp,
    w_up_exp,
    w_down_exp,
    w_gate_shared,
    w_up_shared,
    w_down_shared,
):
    ep, tp = lax.axis_size("ep"), lax.axis_size("tp")
    index = lax.axis_index("tp").astype(jnp.int32)
    exp_dev = w_gate_exp.shape[0]
    experts = exp_dev * ep
    turn_ep = lax.axis_index("ep").astype(jnp.int32)
    meta = jnp.stack([index, turn_ep * exp_dev, turn_ep])
    columns, lines = ep // 2, tp // 2
    rows_second = tokens_second.shape[0]
    whole, half, quarter = pack(meta, tokens_second, ffn_gain, routes, route_weight, experts)
    beside = swap(half, 1, 0)[None]
    around = [swap(quarter, s << 1, 0) for s in range(1, columns)]

    rows_first = tokens_first.shape[0]
    offset = lax.axis_index("ep") * rows_first
    token_positions = (offset + jnp.arange(rows_first, dtype=jnp.int32)).astype(jnp.float32)
    freqs = rope_base ** (-jnp.arange(0, HEAD_SIZE, 2, dtype=jnp.float32) / HEAD_SIZE)
    angles = token_positions[:, None] * jnp.tile(freqs, 2 * LANES // HEAD_SIZE)[None, :]
    wide_kv = key_matrix.shape[1] + value_matrix.shape[1]
    queries, pairs, last = pl.pallas_call(
        project_kernel,
        out_shape=(
            jax.ShapeDtypeStruct((rows_first, w_query.shape[1]), jnp.bfloat16),
            jax.ShapeDtypeStruct((rows_first, wide_kv), jnp.bfloat16),
            jax.ShapeDtypeStruct((BAND_LENGTH, wide_kv), jnp.bfloat16),
        ),
        in_specs=[HBM] * 5 + [VMEM] * 2,
        out_specs=(VMEM,) * 3,
        scratch_shapes=[
            pltpu.VMEM(tokens_first.shape, jnp.bfloat16),
            pltpu.VMEM((1, attn_gain.shape[0]), jnp.float32),
            pltpu.VMEM(w_query.shape, jnp.bfloat16),
            pltpu.VMEM(key_matrix.shape, jnp.bfloat16),
            pltpu.VMEM(value_matrix.shape, jnp.bfloat16),
            pltpu.SemaphoreType.DMA((4 + rows_first // min(128, rows_first),)),
        ],
        cost_estimate=pl.CostEstimate(flops=1 << 30, bytes_accessed=1 << 22, transcendentals=0),
        compiler_params=limit(12),
        name="project",
    )(
        *in_hbm(tokens_first, attn_gain.reshape(1, -1), w_query, key_matrix, value_matrix),
        jnp.cos(angles), jnp.sin(angles),
    )
    before = lax.ppermute(last, "ep", [(i, i + 1) for i in range(ep - 1)])
    count = rows_first // tp
    part = jax.ShapeDtypeStruct((lines, count, w_output.shape[1]), jnp.bfloat16)
    late = (w_gate_shared, w_up_shared, w_down_exp, w_down_shared)
    outward, kept, *late = pl.pallas_call(
        functools.partial(attend_kernel, len(late)),
        out_shape=(part, part, *[pltpu.VMEM(w.shape, w.dtype) for w in late]),
        in_specs=[SMEM] * 2 + [VMEM] * 3 + [HBM] * (1 + len(late)),
        out_specs=(VMEM,) * (2 + len(late)),
        scratch_shapes=[
            pltpu.VMEM((rows_first, w_query.shape[1]), jnp.bfloat16),
            pltpu.VMEM(w_output.shape, jnp.bfloat16),
            pltpu.SemaphoreType.DMA((1 + len(late),)),
        ],
        cost_estimate=pl.CostEstimate(flops=1 << 30, bytes_accessed=1 << 22, transcendentals=0),
        compiler_params=limit(12),
        name="attend",
    )(meta, head_sink_logit, queries, pairs, before, *in_hbm(w_output, *late))
    gate_shared, up_shared, down, down_shared = late
    outward = swap(outward, 0, 1)
    mixer_out = add_up(
        outward[0],
        kept[0],
        *[swap(add_up(outward[s], kept[s]), 0, s << 1) for s in range(1, lines)],
    )
    along = join(around)
    across = swap(along, 1, 0)
    cut = along.shape[2] // LANES // 2 * LANES
    rest_along, rest_across = [(along, 0, 0)], [(across, 0, 0)]
    for s in range(1, lines):
        other = swap(along, 0, s << 1)
        rest_along.append((other, s << 1, 0))
        rest_across.append((swap(other[:, :, :cut], 1, 0), s << 1, 0))
        rest_across.append((swap(across[:, :, cut:], 0, s << 1), s << 1, cut))

    def with_core(listed):
        listed = listed + [(swap(v, 0, 1), x ^ 1, c) for v, x, c in listed]
        return [v for v, _, _ in listed], [(0, x, tp, c) for _, x, c in listed]

    near = ([whole[None], beside, swap(beside, 0, 1)], [(0, None, 1, 0), (1, 0, 2, 0), (1, 1, 2, 0)])
    shared = (gate_shared, up_shared, down_shared)
    keep = []
    for name, (pieces, places), blocks, extra in (
        ("near", near, 2, shared),
        ("across", with_core(rest_across), columns - 1, ()),
        ("along", with_core(rest_along), columns - 1, ()),
    ):
        s, k = experts_call(
            meta, pieces, places, blocks, rows_second,
            w_gate_exp, w_up_exp, down, extra, experts,
        )
        slim = s.shape[-1]
        sent = swap(s, 0, 1).reshape(lines, blocks, rows_second, slim)
        kept = k.reshape(lines, blocks, rows_second, slim)
        spans = [(0, blocks)] if name == "near" else [(1, blocks), (0, 1)]
        gone = [[add_up(sent[i, a:b], kept[i, a:b]) for a, b in spans] for i in range(1, lines)]
        if gone and name == "across":
            meta, gone = lax.optimization_barrier((meta, gone))
        out = [[swap(value, 0, i << 1) for value in gone[i - 1]] for i in range(1, lines)]
        keep.append(
            [
                add_up(sent[0, a:b], kept[0, a:b], *[o[n] for o in out])
                for n, (a, b) in enumerate(spans)
            ]
        )
    near, across, along = keep
    far = [swap(value, 1, 0) for value in across]
    outgoing = [add_up(along[0], far[0])]
    outgoing.append(add_up(along[1], far[1]))
    arrived = [
        swap(outgoing[0][s - 2] if s > 1 else outgoing[1][0], s << 1, 0)
        for s in [*range(2, columns), 1]
    ]
    beside = swap(near[0][1], 1, 0)
    moe_out = add_up(near[0][0], beside, *arrived)
    return (mixer_out, moe_out)


def solution(mesh):
    in_specs = (
        P("ep", None),
        P(),
        P(None, "tp"),
        P(None, "tp"),
        P(None, "tp"),
        P("tp"),
        P("tp", None),
        P("ep", None),
        P(),
        P("ep", None),
        P("ep", None),
        P("ep", None, "tp"),
        P("ep", None, "tp"),
        P("ep", "tp", None),
        P(None, "tp"),
        P(None, "tp"),
        P("tp", None),
    )
    out_specs = (P(("ep", "tp"), None), P("ep", "tp"))

    return jax.shard_map(local, mesh=mesh, in_specs=in_specs, out_specs=out_specs, check_vma=False)
```
